256 devices in a mesh: sp: 64 (over z, x, core), tp: 4 (over y).
Axes of the slice: x: 4, y: 4, z: 8, core: 2. Of those that a mesh axis runs over, the one named last changes fastest.
Arguments:
- conv_in: bfloat16 [49152, 1024], P('sp', 'tp'), may hold values from -6 to 6
- conv_pre: bfloat16 [49152, 1024], P('sp', 'tp'), may hold values from -6 to 6
- conv_post: bfloat16 [49152, 1024], P('sp', 'tp'), may hold values from -6 to 6
- taps: float32 [3, 1024], P(None, 'tp'), may hold values from -3 to 3
- out_proj: bfloat16 [1024, 2048], P('tp'), may hold values from -0.1875 to 0.1875
- stream: bfloat16 [49152, 2048], P(('sp', 'tp')), may hold values from -6 to 6
- norm_gain: float32 [2048], replicated, may hold values from 0.1 to 1.9
- routes: int32 [49152, 2], P(('sp', 'tp')), may hold values from 0 to 63, all different within a row; in each aligned block of 192 rows (0 to 191, 192 to 383, ...) at most 8 rows name the same one
- route_weight: float32 [49152, 2], P(('sp', 'tp')), may hold values from 0.1 to 1
- gate_w: bfloat16 [64, 2048, 2048], P('sp', None, 'tp'), may hold values from -0.52734375 to 0.52734375
- up_w: bfloat16 [64, 2048, 2048], P('sp', None, 'tp'), may hold values from -0.52734375 to 0.52734375
- down_w: bfloat16 [64, 2048, 2048], P('sp', 'tp'), may hold values from -0.013244629 to 0.013244629
Outputs:
- output: bfloat16 [49152, 2048], P(('sp', 'tp'))
The draws below stay inside these ranges and needn't reach their ends.
Inputs may be any that keep to these rules, and one draw needn't show every extreme that they name: `routes`: each row names 2 different experts. In each aligned block of 192 rows no expert is named more than 8 times, a bound that some block reaches.
All inputs are finite; a program needn't handle non-finite values.
Results may differ from the reference program's by a relative error of at most 0.015.
Values may be sent and summed in bfloat16 or wider, within the bound.
No kernel may reach another device: no remote copies, remote signals or barrier semaphores. Data moves between devices by JAX's collectives and lax.ppermute only.
A program may use at most 128 MiB of HBM per device.

```python
import math
import jax
import jax.numpy as jnp
import numpy as np
from jax import lax

D = 2048
CONV = 1024
FF = 2048
TOP = 2
EXPERTS = 64
TOK_DEV = 192
CAP = 8
TOKENS = 49152
N_TP = 4


def block_levels(rng, shape, pieces, low, top_value):
    level = 1.0
    for axis_at, parts in pieces:
        draws = jax.random.uniform(jax.random.fold_in(jax.random.fold_in(rng, 6), axis_at), (parts,), jnp.float32, low / len(pieces), top_value / len(pieces))
        level = level * jnp.repeat(jnp.exp(draws), shape[axis_at] // parts).reshape((-1,) + (1,) * (len(shape) - 1 - axis_at))
    return level


def deal_out(stream_key, own, number, rows, number_of, top, limit, lean):
    sequence = jax.random.permutation(stream_key, number_of)
    crowded, ordinary = load_shares(number_of, rows * top, limit, lean, True), load_shares(number_of, rows * top, limit, lean, False)
    places = jnp.arange(number_of)

    def named(tallies, offset_by):
        used = int((tallies > 0).sum())
        fixed = max(1, used // 4)
        moved = fixed + (places - fixed + offset_by * (used - fixed)) % max(1, number_of - fixed)
        return jnp.zeros((number_of,), jnp.int32).at[sequence[jnp.where(places < fixed, places, moved)]].set(jnp.asarray(tallies, jnp.int32))

    tallies = jnp.where(number % 4 == 0, named(crowded, number // 4), named(ordinary, number - number // 4 - 1))
    mixed = jax.random.permutation(jax.random.fold_in(own, 3), number_of)
    donor, sink = mixed[0:number_of // 2 * 2:2], mixed[1:number_of // 2 * 2:2]
    room = jnp.minimum(tallies[donor] - 1, limit - tallies[sink]) // 2
    room = jnp.where((donor == sequence[0]) | (sink == sequence[0]) | (tallies[sink] == 0), 0, jnp.maximum(room, 0))
    moved = jax.random.randint(jax.random.fold_in(own, 4), (number_of // 2,), 0, 1 << 20) % (room + 1)
    tallies = tallies.at[donor].add(-moved).at[sink].add(moved)
    items = jnp.searchsorted(jnp.cumsum(tallies), jnp.arange(rows * top), side="right").astype(jnp.int32)
    grid = items.reshape(top, rows).T
    grid = grid[jax.random.permutation(jax.random.fold_in(own, 1), rows)]
    offset_by = jax.random.randint(jax.random.fold_in(own, 2), (rows, 1), 0, top)
    return jnp.take_along_axis(grid, (jnp.arange(top)[None, :] + offset_by) % top, axis=1)


def load_shares(amount, total, most, lean, full):
    portions = [(1 << 20) // math.isqrt(standing ** lean) + 1 for standing in range(1, amount + 1)]
    largest = most if full else min(most, max(-(-total // amount), total * portions[0] // sum(portions)))
    least = 1 if total - largest >= amount - 1 else 0
    holding, rest = [largest] + [least] * (amount - 1), total - largest - least * (amount - 1)
    while rest > 0:
        candidates = [i for i in range(1, amount) if holding[i] < largest] or [i for i in range(1, amount) if holding[i] < most]
        pool, budget = sum([portions[i] for i in candidates]), rest
        for i in candidates:
            more = min(most - holding[i], max(1, budget * portions[i] // pool), rest)
            holding[i] = holding[i] + more
            rest = rest - more
    return np.array(holding)


def centred(key, extent, width, bound, pieces=(), kind=jnp.bfloat16):
    level = block_levels(key, extent, pieces, -0.22, 0.18) if pieces else 1.0
    array = jax.random.normal(key, extent, jnp.float32) * width * level
    return jnp.minimum(jnp.maximum(array, -bound), bound).astype(kind)


def setup_inputs(seed: int = 0) -> dict:
    key_of = jax.random.split(jax.random.key(seed), 13)
    conv_in = centred(key_of[0], (TOKENS, CONV), 1.0, 6.0, ((0, 64), (1, 4)))
    conv_pre = centred(key_of[1], (TOKENS, CONV), 1.0, 6.0, ((0, 64), (1, 4)))
    conv_post = centred(key_of[2], (TOKENS, CONV), 1.0, 6.0, ((0, 64), (1, 4)))
    taps = centred(key_of[3], (3, CONV), 0.58, 3.0, ((1, 4),), jnp.float32)
    out_proj = centred(key_of[4], (CONV, D), CONV ** -0.5, 0.1875, ((0, 4),))
    stream = centred(key_of[5], (TOKENS, D), 1.0, 6.0, ((0, 256),))
    norm_gain = jnp.clip(1.0 + 0.18 * jax.random.normal(key_of[6], (D,), jnp.float32), 0.1, 1.9)
    routes_keys = jax.random.split(jax.random.fold_in(key_of[7], 1), TOKENS // TOK_DEV)
    routes_turns = jax.random.permutation(jax.random.fold_in(key_of[7], 3), TOKENS // TOK_DEV)
    routes = jax.vmap(lambda own, number: deal_out(jax.random.fold_in(key_of[7], 2), own, number, TOK_DEV, EXPERTS, TOP, CAP, 1))(routes_keys, routes_turns).reshape((TOKENS, TOP))
    route_weight = jnp.clip(jnp.exp(math.log(1.0) - 2.3025851 * jax.random.uniform(key_of[8], (TOKENS, TOP), jnp.float32) ** block_levels(key_of[8], (TOKENS, TOP), ((0, 256),), -0.2, 0.2)), 0.1, 1.0)
    gate_w = centred(key_of[9], (EXPERTS, D, FF), (4 * D ** -0.5), 0.52734375, ((0, 64), (2, 4)))
    up_w = centred(key_of[10], (EXPERTS, D, FF), (4 * D ** -0.5), 0.52734375, ((0, 64), (2, 4)))
    down_w = centred(key_of[11], (EXPERTS, FF, D), (0.1 * FF ** -0.5), 0.013244629, ((0, 64), (1, 4)))
    return {"conv_in": conv_in, "conv_pre": conv_pre, "conv_post": conv_post, "taps": taps, "out_proj": out_proj, "stream": stream, "norm_gain": norm_gain, "routes": routes, "route_weight": route_weight, "gate_w": gate_w, "up_w": up_w, "down_w": down_w}


EPSILON = 1e-05
LIMIT = 7.0
ALPHA = 1.702

def clamped_unit(gate_pre, up_pre):
    gated = jnp.minimum(gate_pre, LIMIT)
    upward = jnp.clip(up_pre, -LIMIT, LIMIT)
    return (upward + 1.0) * gated * jax.nn.sigmoid(ALPHA * gated)

def block_ranks(chosen, block_rows, count):
    shaped = chosen.reshape(-1, block_rows)
    onehot = (shaped[:, :, None] == jnp.arange(count, dtype=jnp.int32)[None, None, :]).astype(jnp.int32)
    running = jnp.cumsum(onehot, axis=1) - 1
    return lax.optimization_barrier(jnp.sum(running * onehot, axis=2)).reshape(-1).astype(jnp.int32)

def reference(conv_in, conv_pre, conv_post, taps, out_proj, stream, norm_gain, routes, route_weight, gate_w, up_w, down_w):
    product = conv_pre.astype(jnp.float32) * conv_in.astype(jnp.float32)
    padded = jnp.pad(product, ((1, 1), (0, 0)))
    convolved = taps[0] * padded[:-2] + taps[1] * padded[1:-1] + taps[2] * padded[2:]
    mixed = (conv_post.astype(jnp.float32) * convolved).astype(jnp.bfloat16)
    branch = jnp.dot(mixed, out_proj, preferred_element_type=jnp.float32)
    resid = (stream.astype(jnp.float32) + branch).astype(jnp.bfloat16)
    resid_f = resid.astype(jnp.float32)
    scale = lax.rsqrt(lax.optimization_barrier(jnp.mean(resid_f * resid_f, axis=-1, keepdims=True)) + EPSILON)
    normed = (resid_f * scale * norm_gain).astype(jnp.bfloat16)
    chosen = routes.reshape(-1)
    ranks = block_ranks(chosen, TOK_DEV * TOP, EXPERTS)
    entry_ids = jnp.arange(chosen.shape[0], dtype=jnp.int32)
    slot_ids = entry_ids // (TOK_DEV * TOP) * CAP + ranks
    token_ids = entry_ids // TOP
    slots_all = TOKENS // TOK_DEV * CAP
    buffer = jnp.zeros((EXPERTS, slots_all, D), jnp.bfloat16).at[chosen, slot_ids].set(normed[token_ids])
    part_width = FF // N_TP

    def expert_pass(operands):
        rows_in, gate_one, up_one, down_one = operands
        gate_pre = jnp.dot(rows_in, gate_one, preferred_element_type=jnp.float32)
        up_pre = jnp.dot(rows_in, up_one, preferred_element_type=jnp.float32)
        active = clamped_unit(gate_pre, up_pre).astype(jnp.bfloat16)
        summed = jnp.zeros((rows_in.shape[0], D), jnp.float32)
        for portion in range(N_TP):
            lower = portion * part_width
            piece = jnp.dot(active[:, lower:lower + part_width], down_one[lower:lower + part_width], preferred_element_type=jnp.float32).astype(jnp.bfloat16)
            summed = summed + piece.astype(jnp.float32)
        return summed.astype(jnp.bfloat16)
    results = lax.map(expert_pass, (buffer, gate_w, up_w, down_w))
    picked = results[chosen, slot_ids].reshape(TOKENS, TOP, D)
    total = resid.astype(jnp.float32)
    for column in range(TOP):
        total = total + route_weight[:, column:column + 1] * picked[:, column].astype(jnp.float32)
    return total.astype(jnp.bfloat16)
```

```python
import jax
import jax.numpy as jnp
from jax import lax
from jax.sharding import PartitionSpec as P

EPSILON = 1e-05
LIMIT = 7.0
ALPHA = 1.702
SLOTS = 8
CHUNKS = (4, 4)


def shift(x, by):
    count = lax.axis_size("tp")
    return lax.ppermute(x, "tp", [(i, (i + by) % count) for i in range(count)])


def core_swap(x):
    return lax.ppermute(x, "sp", [(i, i ^ 1) for i in range(lax.axis_size("sp"))])


def ring_gather(x):
    half = x.shape[0] // 2
    after = shift(x, -1)
    before = shift(x, 1)
    top = shift(after[:half], -1)
    bottom = shift(before[half:], 1)
    return x, after, (top, bottom), before


def after_all(x, *others):
    return lax.optimization_barrier((x,) + others)[0]


def dot(a, b):
    return jnp.dot(a, b, preferred_element_type=jnp.float32)


def clamped_unit(gate_pre, up_pre):
    gated = jnp.minimum(gate_pre, LIMIT)
    upward = jnp.clip(up_pre, -LIMIT, LIMIT)
    return (upward + 1.0) * gated * jax.nn.sigmoid(ALPHA * gated)


def slots_of(routes, experts):
    rows = routes.shape[0]
    ids = jnp.arange(experts, dtype=jnp.int32)
    first = routes[:, 0:1] == ids
    second = routes[:, 1:2] == ids
    named = (first | second).astype(jnp.bfloat16)
    at = jnp.arange(rows, dtype=jnp.int32)
    earlier = (at[:, None] > at[None, :]).astype(jnp.bfloat16)
    rank = dot(earlier, named)
    ranks = [
        jnp.sum(jnp.where(mine, rank, 0.0), axis=1).astype(jnp.int32) for mine in (first, second)
    ]
    return [routes[:, k] for k in range(2)], ranks


def local(
    conv_in,
    conv_pre,
    conv_post,
    taps,
    out_proj,
    stream,
    norm_gain,
    routes,
    route_weight,
    gate_w,
    up_w,
    down_w,
):
    sp = lax.axis_size("sp")
    tp = lax.axis_size("tp")
    me = lax.axis_index("tp")
    core = lax.axis_index("sp") % 2
    experts = gate_w.shape[0] * sp
    own_rows, width = stream.shape
    channels = conv_in.shape[1]
    lanes = channels // 2

    mine = lax.dynamic_slice_in_dim(out_proj, core * lanes, lanes, axis=0)
    theirs = lax.dynamic_slice_in_dim(out_proj, (1 - core) * lanes, lanes, axis=0)
    proj = ring_gather(mine)

    edge = jnp.stack([conv_in, conv_pre])
    up = [(i, i + 1) for i in range(sp - 1)]
    before = lax.ppermute(edge[:, -1:], "sp", up)
    after = lax.ppermute(edge[:, :1], "sp", [(j, i) for i, j in up])
    f32 = jnp.float32
    product = conv_pre.astype(f32) * conv_in.astype(f32)
    padded = jnp.concatenate(
        [
            before[0].astype(f32) * before[1].astype(f32),
            product,
            after[0].astype(f32) * after[1].astype(f32),
        ]
    )
    convolved = taps[0] * padded[:-2] + taps[1] * padded[1:-1] + taps[2] * padded[2:]
    mixed = (conv_post.astype(f32) * convolved).astype(jnp.bfloat16)
    low, high = mixed[:, :lanes], mixed[:, lanes:]
    mixed = jnp.concatenate(
        [jnp.where(core == 0, low, high), jnp.where(core == 0, high, low)], axis=1
    )

    def rows_for(d):
        return lax.dynamic_slice_in_dim(mixed, ((me - d) % tp) * own_rows, own_rows, axis=0)

    pieces = [rows_for(0)] + [shift(rows_for(d), -d) for d in range(1, tp)]
    half = lanes // 2
    branch = dot(pieces[0][:, :lanes], mine) + dot(pieces[0][:, lanes:], theirs)
    for d in range(1, tp):
        if d == 2:
            for part in range(2):
                cut = slice(part * half, (part + 1) * half)
                cut_b = slice(lanes + part * half, lanes + (part + 1) * half)
                branch += dot(pieces[d][:, cut], proj[d][part])
                branch += dot(pieces[d][:, cut_b], core_swap(proj[d][part]))
        else:
            branch += dot(pieces[d][:, :lanes], proj[d])
            branch += dot(pieces[d][:, lanes:], core_swap(proj[d]))

    down = ring_gather(after_all(down_w[0], proj[1], proj[3], *proj[2], *pieces))
    down = (down[0], down[1], jnp.concatenate(down[2]), down[3])

    resid = (stream.astype(f32) + branch).astype(jnp.bfloat16)
    resid_f = resid.astype(f32)
    scale = lax.rsqrt(jnp.mean(resid_f * resid_f, axis=-1, keepdims=True) + EPSILON)
    normed = (resid_f * scale * norm_gain).astype(jnp.bfloat16)

    expert_of, rank_of = slots_of(routes, experts)

    def dispatch(first, size):
        ids = jnp.arange(experts * size, dtype=jnp.int32)
        picks = []
        for k in range(2):
            local_rank = rank_of[k] - first
            inside = (local_rank >= 0) & (local_rank < size)
            picks.append(jnp.where(inside, expert_of[k] * size + local_rank, -1))
        onehot = ((ids[:, None] == picks[0]) | (ids[:, None] == picks[1])).astype(jnp.bfloat16)
        rows = dot(onehot, normed).astype(jnp.bfloat16).reshape(experts, size, width)
        arrived = lax.all_to_all(rows, "sp", split_axis=0, concat_axis=0, tiled=True)
        return picks, arrived.reshape(experts * size, width)

    def expert(rows):
        active = clamped_unit(dot(rows, gate_w[0]), dot(rows, up_w[0]))
        return active.astype(jnp.bfloat16)

    def give_back(arrived, size):
        own, nxt, opposite, prev = ring_gather(arrived)
        back = [
            expert(own),
            shift(expert(prev), -1),
            shift(expert(jnp.concatenate(opposite)), 2),
            shift(expert(nxt), 1),
        ]
        out = dot(back[0], down[0])
        for d in range(1, tp):
            out += dot(back[d], down[d])
        out = out.astype(jnp.bfloat16).reshape(experts, size, width)
        returned = lax.all_to_all(out, "sp", split_axis=0, concat_axis=0, tiled=True)
        return returned.reshape(experts * size, width)

    sent = []
    first = 0
    for size in CHUNKS:
        sent.append(dispatch(first, size))
        first += size
    picked = [0.0, 0.0]
    for size, (picks, arrived) in zip(CHUNKS, sent):
        returned = give_back(arrived, size)
        ids = jnp.arange(experts * size, dtype=jnp.int32)
        for k in range(2):
            onehot = (picks[k][:, None] == ids[None, :]).astype(jnp.bfloat16)
            picked[k] = picked[k] + dot(onehot, returned)
    total = resid_f
    for k in range(2):
        total = total + route_weight[:, k : k + 1] * picked[k]
    return total.astype(jnp.bfloat16)


def solution(mesh):
    placed = (
        P("sp", "tp"),
        P("sp", "tp"),
        P("sp", "tp"),
        P(None, "tp"),
        P("tp", None),
        P(("sp", "tp"), None),
        P(),
        P(("sp", "tp"), None),
        P(("sp", "tp"), None),
        P("sp", None, "tp"),
        P("sp", None, "tp"),
        P("sp", "tp", None),
    )
    return jax.shard_map(
        local, mesh=mesh, in_specs=placed, out_specs=P(("sp", "tp"), None), check_vma=False
    )
```

```python
import jax
import jax.numpy as jnp
from jax import lax
from jax.sharding import PartitionSpec as P


EPSILON = 1e-05
LIMIT = 7.0
ALPHA = 1.702
CHUNKS = (4, 4)


def shift(x, by):
    count = lax.axis_size("tp")
    return lax.ppermute(x, "tp", [(i, (i + by) % count) for i in range(count)])


def core_swap(x):
    return lax.ppermute(x, "sp", [(i, i ^ 1) for i in range(lax.axis_size("sp"))])


def both(x, pairs):
    sp, tp = lax.axis_size("sp"), lax.axis_size("tp")
    every = []
    for chip in range(sp // 2):
        for (y0, c0), (y1, c1) in pairs:
            every.append(((2 * chip + c0) * tp + y0, (2 * chip + c1) * tp + y1))
    return lax.ppermute(x, ("sp", "tp"), every)


def roles(tp):
    host = [(y, y % 2) for y in range(tp)]
    guest = [(y, 1 - y % 2) for y in range(tp)]
    return host, guest


def weights_to_hosts(low, high):
    tp = lax.axis_size("tp")
    host, guest = roles(tp)
    stay = [(h, h) for h in host]
    to_left = stay + [(guest[y], guest[(y - 1) % tp]) for y in range(tp)]
    to_right = stay + [(guest[y], guest[(y + 1) % tp]) for y in range(tp)]
    return [both(w, to_left) for w in low], [both(w, to_right) for w in high]


def row_routes(tp):
    host, guest = roles(tp)
    first = [(guest[y], host[(y - 1) % tp]) for y in range(tp)]
    first += [(host[y], guest[(y + 2) % tp]) for y in range(tp)]
    second = [(guest[y], guest[(y + 1) % tp]) for y in range(tp)]
    second += [(h, h) for h in host]
    return first, second


def flipped(pairs):
    return [(b, a) for a, b in pairs]


def dot(a, b):
    return jnp.dot(a, b, preferred_element_type=jnp.float32)


def clamped_unit(gate_pre, up_pre):
    gated = jnp.minimum(gate_pre, LIMIT)
    upward = jnp.clip(up_pre, -LIMIT, LIMIT)
    return (upward + 1.0) * gated * jax.nn.sigmoid(ALPHA * gated)


def slots_of(routes, experts):
    rows = routes.shape[0]
    ids = jnp.arange(experts, dtype=jnp.int32)
    first = routes[:, 0:1] == ids
    second = routes[:, 1:2] == ids
    named = (first | second).astype(jnp.bfloat16)
    at = jnp.arange(rows, dtype=jnp.int32)
    earlier = (at[:, None] > at[None, :]).astype(jnp.bfloat16)
    rank = dot(earlier, named)
    ranks = [
        jnp.sum(jnp.where(mine, rank, 0.0), axis=1).astype(jnp.int32) for mine in (first, second)
    ]
    return [routes[:, k] for k in range(2)], ranks


def layer(
    conv_in,
    conv_pre,
    conv_post,
    taps,
    out_proj,
    stream,
    norm_gain,
    routes,
    route_weight,
    gate_w,
    up_w,
    down_w,
):
    sp = lax.axis_size("sp")
    tp = lax.axis_size("tp")
    me = lax.axis_index("tp")
    core = lax.axis_index("sp") % 2
    experts = gate_w.shape[0] * sp
    own_rows, width = stream.shape
    channels = conv_in.shape[1]
    lanes = channels // 2

    mine = lax.dynamic_slice_in_dim(out_proj, core * lanes, lanes, axis=0)
    theirs = lax.dynamic_slice_in_dim(out_proj, (1 - core) * lanes, lanes, axis=0)
    proj = [mine] + [shift(mine, -d) for d in range(1, tp)]

    edge = jnp.stack([conv_in, conv_pre])
    up = [(i, i + 1) for i in range(sp - 1)]
    before = lax.ppermute(edge[:, -1:], "sp", up)
    after = lax.ppermute(edge[:, :1], "sp", [(j, i) for i, j in up])
    f32 = jnp.float32
    product = conv_pre.astype(f32) * conv_in.astype(f32)
    padded = jnp.concatenate(
        [
            before[0].astype(f32) * before[1].astype(f32),
            product,
            after[0].astype(f32) * after[1].astype(f32),
        ]
    )
    convolved = taps[0] * padded[:-2] + taps[1] * padded[1:-1] + taps[2] * padded[2:]
    mixed = (conv_post.astype(f32) * convolved).astype(jnp.bfloat16)
    low, high = mixed[:, :lanes], mixed[:, lanes:]
    mixed = jnp.concatenate(
        [jnp.where(core == 0, low, high), jnp.where(core == 0, high, low)], axis=1
    )

    def rows_for(d):
        return lax.dynamic_slice_in_dim(mixed, ((me - d) % tp) * own_rows, own_rows, axis=0)

    pieces = [rows_for(0)] + [shift(rows_for(d), -d) for d in range(1, tp)]
    branch = dot(pieces[0][:, :lanes], mine) + dot(pieces[0][:, lanes:], theirs)
    for d in (1, 3, 2):
        branch += dot(pieces[d][:, :lanes], proj[d])
        branch += dot(pieces[d][:, lanes:], core_swap(proj[d]))

    unit = gate_w.shape[2] // 2
    gate, up_, down = lax.optimization_barrier((gate_w[0], up_w[0], down_w[0], *pieces, proj[1]))[:3]
    low, high = weights_to_hosts(
        (jnp.concatenate([gate[:, :unit], up_[:, :unit]], axis=1), down[:unit]),
        (jnp.concatenate([gate[:, unit:], up_[:, unit:]], axis=1), down[unit:]),
    )

    resid = (stream.astype(f32) + branch).astype(jnp.bfloat16)
    resid_f = resid.astype(f32)
    scale = lax.rsqrt(jnp.mean(resid_f * resid_f, axis=-1, keepdims=True) + EPSILON)
    normed = (resid_f * scale * norm_gain).astype(jnp.bfloat16)

    expert_of, rank_of = slots_of(routes, experts)

    def dispatch(first, size):
        ids = jnp.arange(experts * size, dtype=jnp.int32)
        picks = []
        for k in range(2):
            local_rank = rank_of[k] - first
            inside = (local_rank >= 0) & (local_rank < size)
            picks.append(jnp.where(inside, expert_of[k] * size + local_rank, -1))
        onehot = ((ids[:, None] == picks[0]) | (ids[:, None] == picks[1])).astype(jnp.bfloat16)
        rows = dot(onehot, normed).astype(jnp.bfloat16).reshape(experts, size, width)
        arrived = lax.all_to_all(rows, "sp", split_axis=0, concat_axis=0, tiled=True)
        return picks, arrived.reshape(experts * size, width)

    def expert(rows):
        part = 0.0
        for gate_up, down_part in (low, high):
            pre = dot(rows, gate_up)
            active = clamped_unit(pre[:, :unit], pre[:, unit:]).astype(jnp.bfloat16)
            part = part + dot(active, down_part)
        return part

    routes_in = row_routes(tp)

    def give_back(arrived, size):
        rows = arrived.shape[0]
        mine_rows = jnp.concatenate([both(arrived, pairs) for pairs in routes_in])
        their_rows = core_swap(mine_rows)
        my_part = expert(mine_rows)
        other_part = expert(their_rows).astype(jnp.bfloat16)
        their_part = core_swap(other_part)
        pair_sum = (my_part + their_part.astype(f32)).astype(jnp.bfloat16)
        halves = [
            both(pair_sum[k * rows : (k + 1) * rows], flipped(pairs))
            for k, pairs in enumerate(routes_in)
        ]
        out = (halves[0].astype(f32) + halves[1].astype(f32)).astype(jnp.bfloat16)
        out = out.reshape(experts, size, width)
        returned = lax.all_to_all(out, "sp", split_axis=0, concat_axis=0, tiled=True)
        return returned.reshape(experts * size, width)

    sent = []
    first = 0
    for size in CHUNKS:
        sent.append(dispatch(first, size))
        first += size
    picked = [0.0, 0.0]
    for size, (picks, arrived) in zip(CHUNKS, sent):
        returned = give_back(arrived, size)
        ids = jnp.arange(experts * size, dtype=jnp.int32)
        for k in range(2):
            onehot = (picks[k][:, None] == ids[None, :]).astype(jnp.bfloat16)
            picked[k] = picked[k] + dot(onehot, returned)
    total = resid_f
    for k in range(2):
        total = total + route_weight[:, k : k + 1] * picked[k]
    return total.astype(jnp.bfloat16)


def solution(mesh):
    placed = (
        P("sp", "tp"),
        P("sp", "tp"),
        P("sp", "tp"),
        P(None, "tp"),
        P("tp", None),
        P(("sp", "tp"), None),
        P(),
        P(("sp", "tp"), None),
        P(("sp", "tp"), None),
        P("sp", None, "tp"),
        P("sp", None, "tp"),
        P("sp", "tp", None),
    )
    return jax.shard_map(
        layer, mesh=mesh, in_specs=placed, out_specs=P(("sp", "tp"), None), check_vma=False
    )
```

```python
import jax
import jax.numpy as jnp
from jax import lax
from jax.experimental import pallas as pl
from jax.experimental.pallas import tpu as pltpu
from jax.sharding import PartitionSpec as P


EPSILON = 1e-05
LIMIT = 7.0
ALPHA = 1.702
CHUNKS = (4, 4)


def shift(x, by):
    count = lax.axis_size("tp")
    return lax.ppermute(x, "tp", [(i, (i + by) % count) for i in range(count)])


def core_swap(x):
    return lax.ppermute(x, "sp", [(i, i ^ 1) for i in range(lax.axis_size("sp"))])


def both(x, pairs):
    sp, tp = lax.axis_size("sp"), lax.axis_size("tp")
    every = []
    for chip in range(sp // 2):
        for (y0, c0), (y1, c1) in pairs:
            every.append(((2 * chip + c0) * tp + y0, (2 * chip + c1) * tp + y1))
    return lax.ppermute(x, ("sp", "tp"), every)


def roles(tp):
    host = [(y, y % 2) for y in range(tp)]
    guest = [(y, 1 - y % 2) for y in range(tp)]
    return host, guest


def weight_routes(tp):
    host, guest = roles(tp)
    over = [(host[y], guest[y]) for y in range(tp)]
    to_left = over + [(guest[y], host[(y - 1) % tp]) for y in range(tp)]
    to_right = over + [(guest[y], host[(y + 1) % tp]) for y in range(tp)]
    return to_left, to_right


def row_routes(tp):
    host, guest = roles(tp)
    first = [(guest[y], host[(y - 1) % tp]) for y in range(tp)]
    first += [(host[y], guest[(y + 2) % tp]) for y in range(tp)]
    second = [(guest[y], host[(y + 1) % tp]) for y in range(tp)]
    second += [(host[y], guest[y]) for y in range(tp)]
    return first, second


def flipped(pairs):
    return [(b, a) for a, b in pairs]


def dot(a, b):
    return jnp.dot(a, b, preferred_element_type=jnp.float32)


def clamped_unit(gate_pre, up_pre):
    gated = jnp.minimum(gate_pre, LIMIT)
    upward = jnp.clip(up_pre, -LIMIT, LIMIT)
    return (upward + 1.0) * gated * jax.nn.sigmoid(ALPHA * gated)


def ffn_kernel(one, two, gu_low, gu_high, down_low, down_high, out_one, out_two):
    unit = down_low.shape[0]
    tile = 256

    def run(rows_ref, out_ref):
        @pl.loop(0, rows_ref.shape[0] // tile)
        def _(step):
            at = pl.ds(pl.multiple_of(step * tile, tile), tile)
            rows = rows_ref[at, :]
            total = None
            for gu, down in ((gu_low, down_low), (gu_high, down_high)):
                pre = dot(rows, gu[...])
                active = clamped_unit(pre[:, :unit], pre[:, unit:]).astype(jnp.bfloat16)
                part = dot(active, down[...])
                total = part if total is None else total + part
            out_ref[at, :] = total.astype(out_ref.dtype)

    run(one, out_one)
    run(two, out_two)


def ffn(one, two, low, high):
    rows, width = one.shape
    unit = low[1].shape[0]
    shape = jax.ShapeDtypeStruct((rows, width), jnp.bfloat16)
    return pl.pallas_call(
        ffn_kernel,
        out_shape=(shape, shape),
        in_specs=[pl.BlockSpec(memory_space=pltpu.VMEM)] * 6,
        out_specs=(pl.BlockSpec(memory_space=pltpu.VMEM),) * 2,
        compiler_params=pltpu.CompilerParams(vmem_limit_bytes=32 * 2**20),
        cost_estimate=pl.CostEstimate(
            flops=2 * 2 * rows * width * 6 * unit,
            bytes_accessed=2 * (4 * rows * width + 6 * unit * width),
            transcendentals=4 * rows * unit,
        ),
    )(one, two, low[0], high[0], low[1], high[1])


def slots_of(routes, experts):
    rows = routes.shape[0]
    ids = jnp.arange(experts, dtype=jnp.int32)
    first = routes[:, 0:1] == ids
    second = routes[:, 1:2] == ids
    named = (first | second).astype(jnp.bfloat16)
    at = jnp.arange(rows, dtype=jnp.int32)
    earlier = (at[:, None] > at[None, :]).astype(jnp.bfloat16)
    rank = dot(earlier, named)
    ranks = [
        jnp.sum(jnp.where(mine, rank, 0.0), axis=1).astype(jnp.int32) for mine in (first, second)
    ]
    return [routes[:, k] for k in range(2)], ranks


def layer(
    conv_in,
    conv_pre,
    conv_post,
    taps,
    out_proj,
    stream,
    norm_gain,
    routes,
    route_weight,
    gate_w,
    up_w,
    down_w,
):
    sp = lax.axis_size("sp")
    tp = lax.axis_size("tp")
    me = lax.axis_index("tp")
    core = lax.axis_index("sp") % 2
    experts = gate_w.shape[0] * sp
    own_rows, width = stream.shape
    channels = conv_in.shape[1]
    lanes = channels // 2

    mine = lax.dynamic_slice_in_dim(out_proj, core * lanes, lanes, axis=0)
    theirs = lax.dynamic_slice_in_dim(out_proj, (1 - core) * lanes, lanes, axis=0)
    proj = [mine] + [shift(mine, -d) for d in range(1, tp)]
    unit = gate_w.shape[2] // 2
    halves_of = [
        (jnp.concatenate([gate_w[0, :, cut], up_w[0, :, cut]], axis=1), down_w[0, cut])
        for cut in (slice(0, unit), slice(unit, 2 * unit))
    ]

    edge = jnp.stack([conv_in, conv_pre])
    up = [(i, i + 1) for i in range(sp - 1)]
    before = lax.ppermute(edge[:, -1:], "sp", up)
    after = lax.ppermute(edge[:, :1], "sp", [(j, i) for i, j in up])
    f32 = jnp.float32
    product = conv_pre.astype(f32) * conv_in.astype(f32)
    padded = jnp.concatenate(
        [
            before[0].astype(f32) * before[1].astype(f32),
            product,
            after[0].astype(f32) * after[1].astype(f32),
        ]
    )
    convolved = taps[0] * padded[:-2] + taps[1] * padded[1:-1] + taps[2] * padded[2:]
    mixed = (conv_post.astype(f32) * convolved).astype(jnp.bfloat16)
    low, high = mixed[:, :lanes], mixed[:, lanes:]
    mixed = jnp.concatenate(
        [jnp.where(core == 0, low, high), jnp.where(core == 0, high, low)], axis=1
    )

    def rows_for(d):
        return lax.dynamic_slice_in_dim(mixed, ((me - d) % tp) * own_rows, own_rows, axis=0)

    pieces = [rows_for(0)] + [shift(rows_for(d), -d) for d in range(1, tp)]
    low, high = [
        [both(w, pairs) for w in held] for held, pairs in zip(halves_of, weight_routes(tp))
    ]
    proj_other = [theirs] + [core_swap(w) for w in proj[1:]]
    branch = 0.0
    for d in (0, 1, 3, 2):
        branch += dot(pieces[d][:, :lanes], proj[d])
        branch += dot(pieces[d][:, lanes:], proj_other[d])

    resid = (stream.astype(f32) + branch).astype(jnp.bfloat16)
    resid_f = resid.astype(f32)
    scale = lax.rsqrt(jnp.mean(resid_f * resid_f, axis=-1, keepdims=True) + EPSILON)
    normed = (resid_f * scale * norm_gain).astype(jnp.bfloat16)

    expert_of, rank_of = slots_of(routes, experts)

    def dispatch(first, size):
        ids = jnp.arange(experts * size, dtype=jnp.int32)
        picks = []
        for k in range(2):
            local_rank = rank_of[k] - first
            inside = (local_rank >= 0) & (local_rank < size)
            picks.append(jnp.where(inside, expert_of[k] * size + local_rank, -1))
        onehot = ((ids[:, None] == picks[0]) | (ids[:, None] == picks[1])).astype(jnp.bfloat16)
        rows = dot(onehot, normed).astype(jnp.bfloat16).reshape(experts, size, width)
        arrived = lax.all_to_all(rows, "sp", split_axis=0, concat_axis=0, tiled=True)
        return picks, arrived.reshape(experts * size, width)

    routes_in = row_routes(tp)

    def give_back(arrived, size):
        mine_rows = [both(arrived, pairs) for pairs in routes_in]
        their_rows = [core_swap(x) for x in mine_rows]
        their_out = ffn(*their_rows, low, high)
        my_out = ffn(*mine_rows, low, high)
        met = [core_swap(x) for x in their_out]
        halves = [
            both((a.astype(f32) + b.astype(f32)).astype(jnp.bfloat16), flipped(pairs))
            for a, b, pairs in zip(my_out, met, routes_in)
        ]
        out = (halves[0].astype(f32) + halves[1].astype(f32)).astype(jnp.bfloat16)
        out = out.reshape(experts, size, width)
        returned = lax.all_to_all(out, "sp", split_axis=0, concat_axis=0, tiled=True)
        return returned.reshape(experts * size, width)

    sent = []
    first = 0
    for size in CHUNKS:
        sent.append(dispatch(first, size))
        first += size
    picked = [0.0, 0.0]
    for size, (picks, arrived) in zip(CHUNKS, sent):
        returned = give_back(arrived, size)
        ids = jnp.arange(experts * size, dtype=jnp.int32)
        for k in range(2):
            onehot = (picks[k][:, None] == ids[None, :]).astype(jnp.bfloat16)
            picked[k] = picked[k] + dot(onehot, returned)
    total = resid_f
    for k in range(2):
        total = total + route_weight[:, k : k + 1] * picked[k]
    return total.astype(jnp.bfloat16)


def solution(mesh):
    placed = (
        P("sp", "tp"),
        P("sp", "tp"),
        P("sp", "tp"),
        P(None, "tp"),
        P("tp", None),
        P(("sp", "tp"), None),
        P(),
        P(("sp", "tp"), None),
        P(("sp", "tp"), None),
        P("sp", None, "tp"),
        P("sp", None, "tp"),
        P("sp", "tp", None),
    )
    return jax.shard_map(
        layer, mesh=mesh, in_specs=placed, out_specs=P(("sp", "tp"), None), check_vma=False
    )
```

```python
import jax
import jax.numpy as jnp
from jax import lax
from jax.experimental import pallas as pl
from jax.experimental.pallas import tpu as pltpu
from jax.sharding import PartitionSpec as P


EPSILON = 1e-05
LIMIT = 7.0
ALPHA = 1.702
CHUNKS = (4, 4)


def shift(x, by):
    count = lax.axis_size("tp")
    return lax.ppermute(x, "tp", [(i, (i + by) % count) for i in range(count)])


def core_swap(x):
    return lax.ppermute(x, "sp", [(i, i ^ 1) for i in range(lax.axis_size("sp"))])


def both(x, pairs):
    sp, tp = lax.axis_size("sp"), lax.axis_size("tp")
    every = []
    for chip in range(sp // 2):
        for (y0, c0), (y1, c1) in pairs:
            every.append(((2 * chip + c0) * tp + y0, (2 * chip + c1) * tp + y1))
    return lax.ppermute(x, ("sp", "tp"), every)


def roles(tp):
    host = [(y, y % 2) for y in range(tp)]
    guest = [(y, 1 - y % 2) for y in range(tp)]
    return host, guest


def weight_routes(tp):
    host, guest = roles(tp)
    over = [(host[y], guest[y]) for y in range(tp)]
    to_left = over + [(guest[y], host[(y - 1) % tp]) for y in range(tp)]
    to_right = over + [(guest[y], host[(y + 1) % tp]) for y in range(tp)]
    return to_left, to_right


def row_routes(tp):
    host, guest = roles(tp)
    first = [(guest[y], host[(y - 1) % tp]) for y in range(tp)]
    first += [(host[y], guest[(y + 2) % tp]) for y in range(tp)]
    second = [(guest[y], host[(y + 1) % tp]) for y in range(tp)]
    second += [(host[y], guest[y]) for y in range(tp)]
    return first, second


def flipped(pairs):
    return [(b, a) for a, b in pairs]


def dot(a, b):
    return jnp.dot(a, b, preferred_element_type=jnp.float32)


def clamped_unit(gate_pre, up_pre):
    gated = jnp.minimum(gate_pre, LIMIT)
    upward = jnp.clip(up_pre, -LIMIT, LIMIT)
    return (upward + 1.0) * gated * jax.nn.sigmoid(ALPHA * gated)


def ffn_kernel(one, two, gu_low, gu_high, down_low, down_high, out_one, out_two):
    unit = down_low.shape[0]
    rows = jnp.concatenate([one[...], two[...]], axis=0)
    total = None
    for gu, down in ((gu_low, down_low), (gu_high, down_high)):
        pre = dot(rows, gu[...])
        active = clamped_unit(pre[:, :unit], pre[:, unit:]).astype(jnp.bfloat16)
        part = dot(active, down[...])
        total = part if total is None else total + part
    total = total.astype(jnp.bfloat16)
    out_one[...] = total[: one.shape[0]]
    out_two[...] = total[one.shape[0] :]


def ffn(one, two, low, high):
    rows, width = one.shape
    unit = low[1].shape[0]
    shape = jax.ShapeDtypeStruct((rows, width), jnp.bfloat16)
    return pl.pallas_call(
        ffn_kernel,
        out_shape=(shape, shape),
        in_specs=[pl.BlockSpec(memory_space=pltpu.VMEM)] * 6,
        out_specs=(pl.BlockSpec(memory_space=pltpu.VMEM),) * 2,
        compiler_params=pltpu.CompilerParams(vmem_limit_bytes=32 * 2**20),
        cost_estimate=pl.CostEstimate(
            flops=2 * 2 * rows * width * 6 * unit,
            bytes_accessed=2 * (4 * rows * width + 6 * unit * width),
            transcendentals=4 * rows * unit,
        ),
    )(one, two, low[0], high[0], low[1], high[1])


def slots_of(routes, experts):
    rows = routes.shape[0]
    ids = jnp.arange(experts, dtype=jnp.int32)
    first = routes[:, 0:1] == ids
    second = routes[:, 1:2] == ids
    named = (first | second).astype(jnp.bfloat16)
    at = jnp.arange(rows, dtype=jnp.int32)
    earlier = (at[:, None] > at[None, :]).astype(jnp.bfloat16)
    rank = dot(earlier, named)
    ranks = [
        jnp.sum(jnp.where(mine, rank, 0.0), axis=1).astype(jnp.int32) for mine in (first, second)
    ]
    return [routes[:, k] for k in range(2)], ranks


def layer(
    conv_in,
    conv_pre,
    conv_post,
    taps,
    out_proj,
    stream,
    norm_gain,
    routes,
    route_weight,
    gate_w,
    up_w,
    down_w,
):
    sp = lax.axis_size("sp")
    tp = lax.axis_size("tp")
    me = lax.axis_index("tp")
    core = lax.axis_index("sp") % 2
    experts = gate_w.shape[0] * sp
    own_rows, width = stream.shape
    channels = conv_in.shape[1]
    lanes = channels // 2

    mine = lax.dynamic_slice_in_dim(out_proj, core * lanes, lanes, axis=0)
    theirs = lax.dynamic_slice_in_dim(out_proj, (1 - core) * lanes, lanes, axis=0)
    proj = [mine] + [shift(mine, -d) for d in range(1, tp)]
    unit = gate_w.shape[2] // 2
    halves_of = [
        (jnp.concatenate([gate_w[0, :, cut], up_w[0, :, cut]], axis=1), down_w[0, cut])
        for cut in (slice(0, unit), slice(unit, 2 * unit))
    ]

    edge = jnp.stack([conv_in, conv_pre])
    up = [(i, i + 1) for i in range(sp - 1)]
    before = lax.ppermute(edge[:, -1:], "sp", up)
    after = lax.ppermute(edge[:, :1], "sp", [(j, i) for i, j in up])
    f32 = jnp.float32
    product = conv_pre.astype(f32) * conv_in.astype(f32)
    padded = jnp.concatenate(
        [
            before[0].astype(f32) * before[1].astype(f32),
            product,
            after[0].astype(f32) * after[1].astype(f32),
        ]
    )
    convolved = taps[0] * padded[:-2] + taps[1] * padded[1:-1] + taps[2] * padded[2:]
    mixed = (conv_post.astype(f32) * convolved).astype(jnp.bfloat16)
    low, high = mixed[:, :lanes], mixed[:, lanes:]
    mixed = jnp.concatenate(
        [jnp.where(core == 0, low, high), jnp.where(core == 0, high, low)], axis=1
    )

    def rows_for(d):
        return lax.dynamic_slice_in_dim(mixed, ((me - d) % tp) * own_rows, own_rows, axis=0)

    pieces = [rows_for(0)] + [shift(rows_for(d), -d) for d in range(1, tp)]
    low, high = [
        [both(w, pairs) for w in held] for held, pairs in zip(halves_of, weight_routes(tp))
    ]
    proj_other = [theirs] + [core_swap(w) for w in proj[1:]]
    branch = 0.0
    for d in (0, 1, 3, 2):
        branch += dot(pieces[d][:, :lanes], proj[d])
        branch += dot(pieces[d][:, lanes:], proj_other[d])

    resid = (stream.astype(f32) + branch).astype(jnp.bfloat16)
    resid_f = resid.astype(f32)
    scale = lax.rsqrt(jnp.mean(resid_f * resid_f, axis=-1, keepdims=True) + EPSILON)
    normed = (resid_f * scale * norm_gain).astype(jnp.bfloat16)

    expert_of, rank_of = slots_of(routes, experts)

    def dispatch(first, size):
        ids = jnp.arange(experts * size, dtype=jnp.int32)
        picks = []
        for k in range(2):
            local_rank = rank_of[k] - first
            inside = (local_rank >= 0) & (local_rank < size)
            picks.append(jnp.where(inside, expert_of[k] * size + local_rank, -1))
        onehot = ((ids[:, None] == picks[0]) | (ids[:, None] == picks[1])).astype(jnp.bfloat16)
        rows = dot(onehot, normed).astype(jnp.bfloat16).reshape(experts, size, width)
        arrived = lax.all_to_all(rows, "sp", split_axis=0, concat_axis=0, tiled=True)
        return picks, arrived.reshape(experts * size, width)

    routes_in = row_routes(tp)

    def give_back(arrived, size):
        mine_rows = [both(arrived, pairs) for pairs in routes_in]
        their_rows = [core_swap(x) for x in mine_rows]
        their_out = ffn(*their_rows, low, high)
        met = [core_swap(x) for x in their_out]
        my_out = ffn(*mine_rows, low, high)
        halves = [
            both((a.astype(f32) + b.astype(f32)).astype(jnp.bfloat16), flipped(pairs))
            for a, b, pairs in zip(my_out, met, routes_in)
        ]
        out = (halves[0].astype(f32) + halves[1].astype(f32)).astype(jnp.bfloat16)
        out = out.reshape(experts, size, width)
        returned = lax.all_to_all(out, "sp", split_axis=0, concat_axis=0, tiled=True)
        return returned.reshape(experts * size, width)

    sent = []
    first = 0
    for size in CHUNKS:
        sent.append(dispatch(first, size))
        first += size
    picked = [0.0, 0.0]
    for size, (picks, arrived) in zip(CHUNKS, sent):
        returned = give_back(arrived, size)
        ids = jnp.arange(experts * size, dtype=jnp.int32)
        for k in range(2):
            onehot = (picks[k][:, None] == ids[None, :]).astype(jnp.bfloat16)
            picked[k] = picked[k] + dot(onehot, returned)
    total = resid_f
    for k in range(2):
        total = total + route_weight[:, k : k + 1] * picked[k]
    return total.astype(jnp.bfloat16)


def solution(mesh):
    placed = (
        P("sp", "tp"),
        P("sp", "tp"),
        P("sp", "tp"),
        P(None, "tp"),
        P("tp", None),
        P(("sp", "tp"), None),
        P(),
        P(("sp", "tp"), None),
        P(("sp", "tp"), None),
        P("sp", None, "tp"),
        P("sp", None, "tp"),
        P("sp", "tp", None),
    )
    return jax.shard_map(
        layer, mesh=mesh, in_specs=placed, out_specs=P(("sp", "tp"), None), check_vma=False
    )
```

```python
import jax
import jax.numpy as jnp
from jax import lax
from jax.experimental import pallas as pl
from jax.experimental.pallas import tpu as pltpu
from jax.sharding import PartitionSpec as P


EPSILON = 1e-05
LIMIT = 7.0
ALPHA = 1.702
CHUNKS = (4, 4)


def shift(x, by):
    count = lax.axis_size("tp")
    return lax.ppermute(x, "tp", [(i, (i + by) % count) for i in range(count)])


def core_swap(x):
    return lax.ppermute(x, "sp", [(i, i ^ 1) for i in range(lax.axis_size("sp"))])


def both(x, pairs):
    sp, tp = lax.axis_size("sp"), lax.axis_size("tp")
    every = []
    for chip in range(sp // 2):
        for (y0, c0), (y1, c1) in pairs:
            every.append(((2 * chip + c0) * tp + y0, (2 * chip + c1) * tp + y1))
    return lax.ppermute(x, ("sp", "tp"), every)


def roles(tp):
    host = [(y, y % 2) for y in range(tp)]
    guest = [(y, 1 - y % 2) for y in range(tp)]
    return host, guest


def weight_routes(tp):
    host, guest = roles(tp)
    over = [(host[y], guest[y]) for y in range(tp)]
    to_left = over + [(guest[y], host[(y - 1) % tp]) for y in range(tp)]
    to_right = over + [(guest[y], host[(y + 1) % tp]) for y in range(tp)]
    return to_left, to_right


def row_routes(tp):
    host, guest = roles(tp)
    first = [(guest[y], host[(y - 1) % tp]) for y in range(tp)]
    first += [(host[y], guest[(y + 2) % tp]) for y in range(tp)]
    second = [(guest[y], host[(y + 1) % tp]) for y in range(tp)]
    second += [(host[y], guest[y]) for y in range(tp)]
    return first, second


def flipped(pairs):
    return [(b, a) for a, b in pairs]


def dot(a, b):
    return jnp.dot(a, b, preferred_element_type=jnp.float32)


def clamped_unit(gate_pre, up_pre):
    gated = jnp.minimum(gate_pre, LIMIT)
    upward = jnp.clip(up_pre, -LIMIT, LIMIT)
    return (upward + 1.0) * gated * jax.nn.sigmoid(ALPHA * gated)


def ffn_kernel(one, two, gu_low, gu_high, down_low, down_high, *outs):
    unit = down_low.shape[0]
    rows = jnp.concatenate([one[...], two[...]], axis=0)
    total = None
    for gu, down in ((gu_low, down_low), (gu_high, down_high)):
        pre = dot(rows, gu[...])
        active = clamped_unit(pre[:, :unit], pre[:, unit:]).astype(jnp.bfloat16)
        part = dot(active, down[...])
        total = part if total is None else total + part
    total = total.astype(jnp.bfloat16)
    each = total.shape[0] // len(outs)
    for k, out in enumerate(outs):
        out[...] = total[k * each : (k + 1) * each]


def ffn(one, two, low, high, count):
    rows, width = one.shape
    unit = low[1].shape[0]
    shape = jax.ShapeDtypeStruct((2 * rows // count, width), jnp.bfloat16)
    return pl.pallas_call(
        ffn_kernel,
        out_shape=(shape,) * count,
        in_specs=[pl.BlockSpec(memory_space=pltpu.VMEM)] * 6,
        out_specs=(pl.BlockSpec(memory_space=pltpu.VMEM),) * count,
        compiler_params=pltpu.CompilerParams(vmem_limit_bytes=32 * 2**20),
        cost_estimate=pl.CostEstimate(
            flops=2 * 2 * rows * width * 6 * unit,
            bytes_accessed=2 * (4 * rows * width + 6 * unit * width),
            transcendentals=4 * rows * unit,
        ),
    )(one, two, low[0], high[0], low[1], high[1])


def slots_of(routes, experts):
    rows = routes.shape[0]
    ids = jnp.arange(experts, dtype=jnp.int32)
    first = routes[:, 0:1] == ids
    second = routes[:, 1:2] == ids
    named = (first | second).astype(jnp.bfloat16)
    at = jnp.arange(rows, dtype=jnp.int32)
    earlier = (at[:, None] > at[None, :]).astype(jnp.bfloat16)
    rank = dot(earlier, named)
    ranks = [
        jnp.sum(jnp.where(mine, rank, 0.0), axis=1).astype(jnp.int32) for mine in (first, second)
    ]
    return [routes[:, k] for k in range(2)], ranks


def layer(
    conv_in,
    conv_pre,
    conv_post,
    taps,
    out_proj,
    stream,
    norm_gain,
    routes,
    route_weight,
    gate_w,
    up_w,
    down_w,
):
    sp = lax.axis_size("sp")
    tp = lax.axis_size("tp")
    me = lax.axis_index("tp")
    core = lax.axis_index("sp") % 2
    experts = gate_w.shape[0] * sp
    own_rows, width = stream.shape
    channels = conv_in.shape[1]
    lanes = channels // 2

    mine = lax.dynamic_slice_in_dim(out_proj, core * lanes, lanes, axis=0)
    theirs = lax.dynamic_slice_in_dim(out_proj, (1 - core) * lanes, lanes, axis=0)
    proj = [mine] + [shift(mine, -d) for d in range(1, tp)]
    unit = gate_w.shape[2] // 2
    halves_of = [
        (jnp.concatenate([gate_w[0, :, cut], up_w[0, :, cut]], axis=1), down_w[0, cut])
        for cut in (slice(0, unit), slice(unit, 2 * unit))
    ]

    edge = jnp.stack([conv_in, conv_pre])
    up = [(i, i + 1) for i in range(sp - 1)]
    before = lax.ppermute(edge[:, -1:], "sp", up)
    after = lax.ppermute(edge[:, :1], "sp", [(j, i) for i, j in up])
    f32 = jnp.float32
    product = conv_pre.astype(f32) * conv_in.astype(f32)
    padded = jnp.concatenate(
        [
            before[0].astype(f32) * before[1].astype(f32),
            product,
            after[0].astype(f32) * after[1].astype(f32),
        ]
    )
    convolved = taps[0] * padded[:-2] + taps[1] * padded[1:-1] + taps[2] * padded[2:]
    mixed = (conv_post.astype(f32) * convolved).astype(jnp.bfloat16)
    low, high = mixed[:, :lanes], mixed[:, lanes:]
    mixed = jnp.concatenate(
        [jnp.where(core == 0, low, high), jnp.where(core == 0, high, low)], axis=1
    )

    def rows_for(d):
        return lax.dynamic_slice_in_dim(mixed, ((me - d) % tp) * own_rows, own_rows, axis=0)

    pieces = [rows_for(0)] + [shift(rows_for(d), -d) for d in range(1, tp)]
    low, high = [
        [both(w, pairs) for w in held] for held, pairs in zip(halves_of, weight_routes(tp))
    ]
    proj_other = [theirs] + [core_swap(w) for w in proj[1:]]
    branch = 0.0
    for d in (0, 1, 3, 2):
        branch += dot(pieces[d][:, :lanes], proj[d])
        branch += dot(pieces[d][:, lanes:], proj_other[d])

    resid = (stream.astype(f32) + branch).astype(jnp.bfloat16)
    resid_f = resid.astype(f32)
    scale = lax.rsqrt(jnp.mean(resid_f * resid_f, axis=-1, keepdims=True) + EPSILON)
    normed = (resid_f * scale * norm_gain).astype(jnp.bfloat16)

    expert_of, rank_of = slots_of(routes, experts)

    def dispatch(first, size):
        ids = jnp.arange(experts * size, dtype=jnp.int32)
        picks = []
        for k in range(2):
            local_rank = rank_of[k] - first
            inside = (local_rank >= 0) & (local_rank < size)
            picks.append(jnp.where(inside, expert_of[k] * size + local_rank, -1))
        onehot = ((ids[:, None] == picks[0]) | (ids[:, None] == picks[1])).astype(jnp.bfloat16)
        rows = dot(onehot, normed).astype(jnp.bfloat16).reshape(experts, size, width)
        arrived = lax.all_to_all(rows, "sp", split_axis=0, concat_axis=0, tiled=True)
        return picks, arrived.reshape(experts * size, width)

    routes_in = row_routes(tp)

    def give_back(arrived, size):
        rows = arrived.shape[0]
        mine_rows = [both(arrived, pairs) for pairs in routes_in]
        their_rows = [core_swap(x) for x in mine_rows]
        (their_out,) = ffn(*their_rows, low, high, 1)
        met = core_swap(their_out)
        my_out = ffn(*mine_rows, low, high, 2)
        paired = [
            (a.astype(f32) + b.astype(f32)).astype(jnp.bfloat16)
            for a, b in zip(my_out, (met[:rows], met[rows:]))
        ]
        halves = [both(x, flipped(pairs)) for x, pairs in zip(paired, routes_in)]
        out = (halves[0].astype(f32) + halves[1].astype(f32)).astype(jnp.bfloat16)
        out = out.reshape(experts, size, width)
        returned = lax.all_to_all(out, "sp", split_axis=0, concat_axis=0, tiled=True)
        return returned.reshape(experts * size, width)

    sent = []
    first = 0
    for size in CHUNKS:
        sent.append(dispatch(first, size))
        first += size
    picked = [0.0, 0.0]
    for size, (picks, arrived) in zip(CHUNKS, sent):
        returned = give_back(arrived, size)
        ids = jnp.arange(experts * size, dtype=jnp.int32)
        for k in range(2):
            onehot = (picks[k][:, None] == ids[None, :]).astype(jnp.bfloat16)
            picked[k] = picked[k] + dot(onehot, returned)
    total = resid_f
    for k in range(2):
        total = total + route_weight[:, k : k + 1] * picked[k]
    return total.astype(jnp.bfloat16)


def solution(mesh):
    placed = (
        P("sp", "tp"),
        P("sp", "tp"),
        P("sp", "tp"),
        P(None, "tp"),
        P("tp", None),
        P(("sp", "tp"), None),
        P(),
        P(("sp", "tp"), None),
        P(("sp", "tp"), None),
        P("sp", None, "tp"),
        P("sp", None, "tp"),
        P("sp", "tp", None),
    )
    return jax.shard_map(
        layer, mesh=mesh, in_specs=placed, out_specs=P(("sp", "tp"), None), check_vma=False
    )
```

```python
import jax
import jax.numpy as jnp
from jax import lax
from jax.experimental import pallas as pl
from jax.experimental.pallas import tpu as pltpu
from jax.sharding import PartitionSpec as P


EPSILON = 1e-05
LIMIT = 7.0
ALPHA = 1.702
CHUNKS = (4, 4)


def shift(x, by):
    count = lax.axis_size("tp")
    return lax.ppermute(x, "tp", [(i, (i + by) % count) for i in range(count)])


def core_swap(x):
    return lax.ppermute(x, "sp", [(i, i ^ 1) for i in range(lax.axis_size("sp"))])


def both(x, pairs):
    sp, tp = lax.axis_size("sp"), lax.axis_size("tp")
    every = []
    for chip in range(sp // 2):
        for (y0, c0), (y1, c1) in pairs:
            every.append(((2 * chip + c0) * tp + y0, (2 * chip + c1) * tp + y1))
    return lax.ppermute(x, ("sp", "tp"), every)


def roles(tp):
    host = [(y, y % 2) for y in range(tp)]
    guest = [(y, 1 - y % 2) for y in range(tp)]
    return host, guest


def weight_routes(tp):
    host, guest = roles(tp)
    over = [(host[y], guest[y]) for y in range(tp)]
    to_left = over + [(guest[y], host[(y - 1) % tp]) for y in range(tp)]
    to_right = over + [(guest[y], host[(y + 1) % tp]) for y in range(tp)]
    return to_left, to_right


def row_routes(tp):
    host, guest = roles(tp)
    first = [(guest[y], host[(y - 1) % tp]) for y in range(tp)]
    first += [(host[y], guest[(y + 2) % tp]) for y in range(tp)]
    second = [(guest[y], host[(y + 1) % tp]) for y in range(tp)]
    second += [(host[y], guest[y]) for y in range(tp)]
    return first, second


def flipped(pairs):
    return [(b, a) for a, b in pairs]


def dot(a, b):
    return jnp.dot(a, b, preferred_element_type=jnp.float32)


def clamped_unit(gate_pre, up_pre):
    gated = jnp.minimum(gate_pre, LIMIT)
    upward = jnp.clip(up_pre, -LIMIT, LIMIT)
    return (upward + 1.0) * gated * jax.nn.sigmoid(ALPHA * gated)


def ffn_kernel(one, two, gu_low, gu_high, down_low, down_high, *outs):
    unit = down_low.shape[0]
    rows = jnp.concatenate([one[...], two[...]], axis=0)
    total = None
    for gu, down in ((gu_low, down_low), (gu_high, down_high)):
        pre = dot(rows, gu[...])
        active = clamped_unit(pre[:, :unit], pre[:, unit:]).astype(jnp.bfloat16)
        part = dot(active, down[...])
        total = part if total is None else total + part
    total = total.astype(jnp.bfloat16)
    each = total.shape[0] // len(outs)
    for k, out in enumerate(outs):
        out[...] = total[k * each : (k + 1) * each]


def ffn(one, two, low, high, count):
    rows, width = one.shape
    unit = low[1].shape[0]
    shape = jax.ShapeDtypeStruct((2 * rows // count, width), jnp.bfloat16)
    return pl.pallas_call(
        ffn_kernel,
        out_shape=(shape,) * count,
        in_specs=[pl.BlockSpec(memory_space=pltpu.VMEM)] * 6,
        out_specs=(pl.BlockSpec(memory_space=pltpu.VMEM),) * count,
        compiler_params=pltpu.CompilerParams(vmem_limit_bytes=32 * 2**20),
        cost_estimate=pl.CostEstimate(
            flops=2 * 2 * rows * width * 6 * unit,
            bytes_accessed=2 * (4 * rows * width + 6 * unit * width),
            transcendentals=4 * rows * unit,
        ),
    )(one, two, low[0], high[0], low[1], high[1])


def slots_of(routes, experts):
    rows = routes.shape[0]
    ids = jnp.arange(experts, dtype=jnp.int32)
    first = routes[:, 0:1] == ids
    second = routes[:, 1:2] == ids
    named = (first | second).astype(jnp.bfloat16)
    at = jnp.arange(rows, dtype=jnp.int32)
    earlier = (at[:, None] > at[None, :]).astype(jnp.bfloat16)
    rank = dot(earlier, named)
    ranks = [
        jnp.sum(jnp.where(mine, rank, 0.0), axis=1).astype(jnp.int32) for mine in (first, second)
    ]
    return [routes[:, k] for k in range(2)], ranks


def layer(
    conv_in,
    conv_pre,
    conv_post,
    taps,
    out_proj,
    stream,
    norm_gain,
    routes,
    route_weight,
    gate_w,
    up_w,
    down_w,
):
    sp = lax.axis_size("sp")
    tp = lax.axis_size("tp")
    me = lax.axis_index("tp")
    core = lax.axis_index("sp") % 2
    experts = gate_w.shape[0] * sp
    own_rows, width = stream.shape
    channels = conv_in.shape[1]
    lanes = channels // 2

    mine = lax.dynamic_slice_in_dim(out_proj, core * lanes, lanes, axis=0)
    theirs = lax.dynamic_slice_in_dim(out_proj, (1 - core) * lanes, lanes, axis=0)
    after, before = shift(mine, -1), shift(mine, 1)
    half = lanes // 2
    opposite = jnp.concatenate([shift(after[:half], -1), shift(before[half:], 1)])
    proj = [mine, after, opposite, before]
    unit = gate_w.shape[2] // 2
    halves_of = [
        (jnp.concatenate([gate_w[0, :, cut], up_w[0, :, cut]], axis=1), down_w[0, cut])
        for cut in (slice(0, unit), slice(unit, 2 * unit))
    ]

    edge = jnp.stack([conv_in, conv_pre])
    up = [(i, i + 1) for i in range(sp - 1)]
    prior = lax.ppermute(edge[:, -1:], "sp", up)
    later = lax.ppermute(edge[:, :1], "sp", [(j, i) for i, j in up])
    f32 = jnp.float32
    product = conv_pre.astype(f32) * conv_in.astype(f32)
    padded = jnp.concatenate(
        [
            prior[0].astype(f32) * prior[1].astype(f32),
            product,
            later[0].astype(f32) * later[1].astype(f32),
        ]
    )
    convolved = taps[0] * padded[:-2] + taps[1] * padded[1:-1] + taps[2] * padded[2:]
    mixed = (conv_post.astype(f32) * convolved).astype(jnp.bfloat16)
    low, high = mixed[:, :lanes], mixed[:, lanes:]
    mixed = jnp.concatenate(
        [jnp.where(core == 0, low, high), jnp.where(core == 0, high, low)], axis=1
    )

    def rows_for(d):
        return lax.dynamic_slice_in_dim(mixed, ((me - d) % tp) * own_rows, own_rows, axis=0)

    pieces = [rows_for(0)] + [shift(rows_for(d), -d) for d in range(1, tp)]
    low, high = [
        [both(w, pairs) for w in held] for held, pairs in zip(halves_of, weight_routes(tp))
    ]
    other = {d: core_swap(proj[d]) for d in (1, 3)}
    other[2] = core_swap(opposite)
    other[0] = theirs

    def product_of(d):
        return dot(pieces[d][:, :lanes], proj[d]) + dot(pieces[d][:, lanes:], other[d])

    branch = product_of(0) + product_of(1) + product_of(3)
    branch += product_of(2)

    resid = (stream.astype(f32) + branch).astype(jnp.bfloat16)
    resid_f = resid.astype(f32)
    scale = lax.rsqrt(jnp.mean(resid_f * resid_f, axis=-1, keepdims=True) + EPSILON)
    normed = (resid_f * scale * norm_gain).astype(jnp.bfloat16)

    expert_of, rank_of = slots_of(routes, experts)

    def dispatch(first, size):
        ids = jnp.arange(experts * size, dtype=jnp.int32)
        picks = []
        for k in range(2):
            local_rank = rank_of[k] - first
            inside = (local_rank >= 0) & (local_rank < size)
            picks.append(jnp.where(inside, expert_of[k] * size + local_rank, -1))
        onehot = ((ids[:, None] == picks[0]) | (ids[:, None] == picks[1])).astype(jnp.bfloat16)
        rows = dot(onehot, normed).astype(jnp.bfloat16).reshape(experts, size, width)
        arrived = lax.all_to_all(rows, "sp", split_axis=0, concat_axis=0, tiled=True)
        return picks, arrived.reshape(experts * size, width)

    routes_in = row_routes(tp)

    def give_back(arrived, size):
        rows = arrived.shape[0]
        mine_rows = [both(arrived, pairs) for pairs in routes_in]
        their_rows = [core_swap(x) for x in mine_rows]
        (their_out,) = ffn(*their_rows, low, high, 1)
        met = core_swap(their_out)
        my_out = ffn(*mine_rows, low, high, 2)
        paired = [
            (a.astype(f32) + b.astype(f32)).astype(jnp.bfloat16)
            for a, b in zip(my_out, (met[:rows], met[rows:]))
        ]
        halves = [both(x, flipped(pairs)) for x, pairs in zip(paired, routes_in)]
        out = (halves[0].astype(f32) + halves[1].astype(f32)).astype(jnp.bfloat16)
        out = out.reshape(experts, size, width)
        returned = lax.all_to_all(out, "sp", split_axis=0, concat_axis=0, tiled=True)
        return returned.reshape(experts * size, width)

    sent = []
    first = 0
    for size in CHUNKS:
        sent.append(dispatch(first, size))
        first += size
    picked = [0.0, 0.0]
    for size, (picks, arrived) in zip(CHUNKS, sent):
        returned = give_back(arrived, size)
        ids = jnp.arange(experts * size, dtype=jnp.int32)
        for k in range(2):
            onehot = (picks[k][:, None] == ids[None, :]).astype(jnp.bfloat16)
            picked[k] = picked[k] + dot(onehot, returned)
    total = resid_f
    for k in range(2):
        total = total + route_weight[:, k : k + 1] * picked[k]
    return total.astype(jnp.bfloat16)


def solution(mesh):
    placed = (
        P("sp", "tp"),
        P("sp", "tp"),
        P("sp", "tp"),
        P(None, "tp"),
        P("tp", None),
        P(("sp", "tp"), None),
        P(),
        P(("sp", "tp"), None),
        P(("sp", "tp"), None),
        P("sp", None, "tp"),
        P("sp", None, "tp"),
        P("sp", "tp", None),
    )
    return jax.shard_map(
        layer, mesh=mesh, in_specs=placed, out_specs=P(("sp", "tp"), None), check_vma=False
    )
```

```python
import jax
import jax.numpy as jnp
from jax import lax
from jax.experimental import pallas as pl
from jax.experimental.pallas import tpu as pltpu
from jax.sharding import PartitionSpec as P


EPSILON = 1e-05
LIMIT = 7.0
ALPHA = 1.702
CHUNKS = (4, 4)


def shift(x, by):
    count = lax.axis_size("tp")
    return lax.ppermute(x, "tp", [(i, (i + by) % count) for i in range(count)])


def core_swap(x):
    return lax.ppermute(x, "sp", [(i, i ^ 1) for i in range(lax.axis_size("sp"))])


def both(x, pairs):
    sp, tp = lax.axis_size("sp"), lax.axis_size("tp")
    every = []
    for chip in range(sp // 2):
        for (y0, c0), (y1, c1) in pairs:
            every.append(((2 * chip + c0) * tp + y0, (2 * chip + c1) * tp + y1))
    return lax.ppermute(x, ("sp", "tp"), every)


def roles(tp):
    host = [(y, y % 2) for y in range(tp)]
    guest = [(y, 1 - y % 2) for y in range(tp)]
    return host, guest


def weight_routes(tp):
    host, guest = roles(tp)
    over = [(host[y], guest[y]) for y in range(tp)]
    to_left = over + [(guest[y], host[(y - 1) % tp]) for y in range(tp)]
    to_right = over + [(guest[y], host[(y + 1) % tp]) for y in range(tp)]
    return to_left, to_right


def row_routes(tp):
    host, guest = roles(tp)
    first = [(guest[y], host[(y - 1) % tp]) for y in range(tp)]
    first += [(host[y], guest[(y + 2) % tp]) for y in range(tp)]
    second = [(guest[y], host[(y + 1) % tp]) for y in range(tp)]
    second += [(host[y], guest[y]) for y in range(tp)]
    return first, second


def flipped(pairs):
    return [(b, a) for a, b in pairs]


def dot(a, b):
    return jnp.dot(a, b, preferred_element_type=jnp.float32)


def clamped_unit(gate_pre, up_pre):
    gated = jnp.minimum(gate_pre, LIMIT)
    upward = jnp.clip(up_pre, -LIMIT, LIMIT)
    return (upward + 1.0) * gated * jax.nn.sigmoid(ALPHA * gated)


BLOCK = 256


def blocks(length, size):
    def over(body):
        @pl.loop(0, length // size)
        def _(step):
            body(pl.ds(pl.multiple_of(step * size, size), size))

    return over


def ffn_kernel(rows, gu_low, gu_high, down_low, down_high, *rest):
    *rest, pre, active = rest
    met, outs = (rest[0], rest[1:]) if len(rest) == 3 else (None, rest)
    count, width = rows.shape
    unit = down_low.shape[0]
    each = count // len(outs)

    for k, gu in enumerate((gu_low, gu_high)):

        @blocks(count, 64)
        def _(at):
            pre[at, :] = jnp.zeros((at.size, 2 * unit), jnp.float32)

        @blocks(width, BLOCK)
        def _(at):
            pre[...] += dot(rows[:, at], gu[at, :])

        @blocks(count, 32)
        def _(at):
            active[k, at, :] = clamped_unit(pre[at, :unit], pre[at, unit:]).astype(jnp.bfloat16)

    @blocks(width, BLOCK)
    def _(at):
        total = dot(active[0], down_low[:, at]) + dot(active[1], down_high[:, at])
        if met is not None:
            total = total + met[:, at].astype(jnp.float32)
        total = total.astype(jnp.bfloat16)
        for k, out in enumerate(outs):
            out[:, at] = total[k * each : (k + 1) * each]


def ffn(rows, low, high, met=None):
    number, width = rows.shape
    unit = low[1].shape[0]
    count = 1 if met is None else 2
    shape = jax.ShapeDtypeStruct((number // count, width), jnp.bfloat16)
    operands = (rows, low[0], high[0], low[1], high[1]) + (() if met is None else (met,))
    return pl.pallas_call(
        ffn_kernel,
        out_shape=(shape,) * count,
        in_specs=[pl.BlockSpec(memory_space=pltpu.VMEM)] * len(operands),
        out_specs=(pl.BlockSpec(memory_space=pltpu.VMEM),) * count,
        scratch_shapes=[
            pltpu.VMEM((number, 2 * unit), jnp.float32),
            pltpu.VMEM((2, number, unit), jnp.bfloat16),
        ],
        compiler_params=pltpu.CompilerParams(vmem_limit_bytes=32 * 2**20),
        cost_estimate=pl.CostEstimate(
            flops=2 * number * width * 6 * unit,
            bytes_accessed=4 * number * width + 12 * unit * width,
            transcendentals=2 * number * unit,
        ),
    )(*operands)


def sum_kernel(a, b, out):
    @blocks(a.shape[0], 32)
    def _(at):
        total = a[at, :].astype(jnp.float32) + b[at, :].astype(jnp.float32)
        out[at, :] = total.astype(out.dtype)


def sum_of(a, b):
    return pl.pallas_call(
        sum_kernel,
        out_shape=jax.ShapeDtypeStruct(a.shape, a.dtype),
        in_specs=[pl.BlockSpec(memory_space=pltpu.VMEM)] * 2,
        out_specs=pl.BlockSpec(memory_space=pltpu.VMEM),
        compiler_params=pltpu.CompilerParams(vmem_limit_bytes=8 * 2**20),
        cost_estimate=pl.CostEstimate(
            flops=a.size, bytes_accessed=3 * 2 * a.size, transcendentals=0
        ),
    )(a, b)


def combine_kernel(resid, first, second, places, weight, out, picks):
    shape = picks.shape[1:]
    ids = lax.broadcasted_iota(jnp.int32, shape, 1)
    for at in range(4):
        mine = places[:, at : at + 1] == ids
        picks[at] = jnp.where(mine, 1.0, 0.0).astype(jnp.bfloat16)

    @blocks(resid.shape[1], BLOCK)
    def _(at):
        total = resid[:, at].astype(jnp.float32)
        for k in range(2):
            picked = dot(picks[k], first[:, at]) + dot(picks[2 + k], second[:, at])
            total = total + weight[:, k : k + 1] * picked
        out[:, at] = total.astype(out.dtype)


def combine(resid, first, second, places, weight):
    rows, width = resid.shape
    number = first.shape[0]
    return pl.pallas_call(
        combine_kernel,
        out_shape=jax.ShapeDtypeStruct(resid.shape, resid.dtype),
        in_specs=[pl.BlockSpec(memory_space=pltpu.VMEM)] * 5,
        out_specs=pl.BlockSpec(memory_space=pltpu.VMEM),
        scratch_shapes=[pltpu.VMEM((4, rows, number), jnp.bfloat16)],
        compiler_params=pltpu.CompilerParams(vmem_limit_bytes=16 * 2**20),
        cost_estimate=pl.CostEstimate(
            flops=8 * rows * number * width,
            bytes_accessed=4 * (rows + number) * width,
            transcendentals=0,
        ),
    )(resid, first, second, places, weight)


def fill_kernel(resid, gain, places, *rest):
    *outs, picks = rest
    rows, width = resid.shape
    ids = lax.broadcasted_iota(jnp.int32, picks.shape[1:], 0)
    for c in range(len(outs)):
        mine = (places[2 * c : 2 * c + 1, :] == ids) | (places[2 * c + 1 : 2 * c + 2, :] == ids)
        picks[c] = jnp.where(mine, 1.0, 0.0).astype(jnp.bfloat16)

    def add(step, total):
        at = pl.ds(pl.multiple_of(step * BLOCK, BLOCK), BLOCK)
        part = resid[:, at].astype(jnp.float32)
        return total + jnp.sum(part * part, axis=1, keepdims=True)

    square = lax.fori_loop(0, width // BLOCK, add, jnp.zeros((rows, 1), jnp.float32))
    scale = lax.rsqrt(square / width + EPSILON)

    @blocks(width, BLOCK)
    def _(at):
        normed = resid[:, at].astype(jnp.float32) * scale * gain[:, at]
        normed = normed.astype(jnp.bfloat16)
        for c, out in enumerate(outs):
            out[:, at] = dot(picks[c], normed).astype(out.dtype)


def fill(resid, gain, places, sizes):
    rows, width = resid.shape
    return pl.pallas_call(
        fill_kernel,
        out_shape=tuple(jax.ShapeDtypeStruct((n, width), jnp.bfloat16) for n in sizes),
        in_specs=[pl.BlockSpec(memory_space=pltpu.VMEM)] * 3,
        out_specs=(pl.BlockSpec(memory_space=pltpu.VMEM),) * len(sizes),
        scratch_shapes=[pltpu.VMEM((len(sizes), sizes[0], rows), jnp.bfloat16)],
        compiler_params=pltpu.CompilerParams(vmem_limit_bytes=16 * 2**20),
        cost_estimate=pl.CostEstimate(
            flops=2 * rows * sum(sizes) * width,
            bytes_accessed=2 * (rows + sum(sizes)) * width,
            transcendentals=rows,
        ),
    )(resid, gain, places)


def slots_of(routes, experts):
    rows = routes.shape[0]
    ids = jnp.arange(experts, dtype=jnp.int32)
    first = routes[:, 0:1] == ids
    second = routes[:, 1:2] == ids
    named = (first | second).astype(jnp.bfloat16)
    at = jnp.arange(rows, dtype=jnp.int32)
    earlier = (at[:, None] > at[None, :]).astype(jnp.bfloat16)
    rank = dot(earlier, named)
    ranks = [
        jnp.sum(jnp.where(mine, rank, 0.0), axis=1).astype(jnp.int32) for mine in (first, second)
    ]
    return [routes[:, k] for k in range(2)], ranks


def layer(
    conv_in,
    conv_pre,
    conv_post,
    taps,
    out_proj,
    stream,
    norm_gain,
    routes,
    route_weight,
    gate_w,
    up_w,
    down_w,
):
    sp = lax.axis_size("sp")
    tp = lax.axis_size("tp")
    me = lax.axis_index("tp")
    core = lax.axis_index("sp") % 2
    experts = gate_w.shape[0] * sp
    own_rows, width = stream.shape
    channels = conv_in.shape[1]
    lanes = channels // 2

    mine = lax.dynamic_slice_in_dim(out_proj, core * lanes, lanes, axis=0)
    theirs = lax.dynamic_slice_in_dim(out_proj, (1 - core) * lanes, lanes, axis=0)
    after, before = shift(mine, -1), shift(mine, 1)
    half = lanes // 2
    opposite = jnp.concatenate([shift(after[:half], -1), shift(before[half:], 1)])
    proj = [mine, after, opposite, before]
    unit = gate_w.shape[2] // 2
    halves_of = [
        (jnp.concatenate([gate_w[0, :, cut], up_w[0, :, cut]], axis=1), down_w[0, cut])
        for cut in (slice(0, unit), slice(unit, 2 * unit))
    ]

    edge = jnp.stack([conv_in, conv_pre])
    up = [(i, i + 1) for i in range(sp - 1)]
    prior = lax.ppermute(edge[:, -1:], "sp", up)
    later = lax.ppermute(edge[:, :1], "sp", [(j, i) for i, j in up])
    f32 = jnp.float32
    product = conv_pre.astype(f32) * conv_in.astype(f32)
    padded = jnp.concatenate(
        [
            prior[0].astype(f32) * prior[1].astype(f32),
            product,
            later[0].astype(f32) * later[1].astype(f32),
        ]
    )
    convolved = taps[0] * padded[:-2] + taps[1] * padded[1:-1] + taps[2] * padded[2:]
    mixed = (conv_post.astype(f32) * convolved).astype(jnp.bfloat16)
    low, high = mixed[:, :lanes], mixed[:, lanes:]
    mixed = jnp.concatenate(
        [jnp.where(core == 0, low, high), jnp.where(core == 0, high, low)], axis=1
    )

    def rows_for(d):
        return lax.dynamic_slice_in_dim(mixed, ((me - d) % tp) * own_rows, own_rows, axis=0)

    pieces = [rows_for(0)] + [shift(rows_for(d), -d) for d in range(1, tp)]
    low, high = [
        [both(w, pairs) for w in held] for held, pairs in zip(halves_of, weight_routes(tp))
    ]
    other = {d: core_swap(proj[d]) for d in (1, 3)}
    other[2] = core_swap(opposite)
    other[0] = theirs

    def product_of(d):
        return dot(pieces[d][:, :lanes], proj[d]) + dot(pieces[d][:, lanes:], other[d])

    branch = product_of(0) + product_of(1) + product_of(3)
    branch += product_of(2)

    resid = (stream.astype(f32) + branch).astype(jnp.bfloat16)
    expert_of, rank_of = slots_of(routes, experts)

    firsts = [sum(CHUNKS[:at]) for at in range(len(CHUNKS))]
    places = []
    for first, size in zip(firsts, CHUNKS):
        for e, r in zip(expert_of, rank_of):
            inside = (r >= first) & (r < first + size)
            places.append(jnp.where(inside, e * size + r - first, -1))
    filled = fill(resid, norm_gain[None, :], jnp.stack(places), [experts * size for size in CHUNKS])

    def dispatch(rows, size):
        rows = rows.reshape(experts, size, width)
        arrived = lax.all_to_all(rows, "sp", split_axis=0, concat_axis=0, tiled=True)
        return arrived.reshape(experts * size, width)

    routes_in = row_routes(tp)

    def give_back(arrived, size):
        mine_rows = jnp.concatenate([both(arrived, pairs) for pairs in routes_in])
        their_rows = core_swap(mine_rows)
        (their_out,) = ffn(their_rows, low, high)
        met = core_swap(their_out)
        paired = ffn(mine_rows, low, high, met)
        halves = [both(x, flipped(pairs)) for x, pairs in zip(paired, routes_in)]
        out = sum_of(*halves)
        out = out.reshape(experts, size, width)
        returned = lax.all_to_all(out, "sp", split_axis=0, concat_axis=0, tiled=True)
        return returned.reshape(experts * size, width)

    sent = [dispatch(rows, size) for rows, size in zip(filled, CHUNKS)]
    returned = [give_back(arrived, size) for arrived, size in zip(sent, CHUNKS)]
    return combine(resid, *returned, jnp.stack(places, axis=1), route_weight)


def solution(mesh):
    placed = (
        P("sp", "tp"),
        P("sp", "tp"),
        P("sp", "tp"),
        P(None, "tp"),
        P("tp", None),
        P(("sp", "tp"), None),
        P(),
        P(("sp", "tp"), None),
        P(("sp", "tp"), None),
        P("sp", None, "tp"),
        P("sp", None, "tp"),
        P("sp", "tp", None),
    )
    return jax.shard_map(
        layer, mesh=mesh, in_specs=placed, out_specs=P(("sp", "tp"), None), check_vma=False
    )
```

```python
import jax
import jax.numpy as jnp
from jax import lax
from jax.experimental import pallas as pl
from jax.experimental.pallas import tpu as pltpu
from jax.sharding import PartitionSpec as P


EPSILON = 1e-05
LIMIT = 7.0
ALPHA = 1.702
CHUNKS = (4, 4)


def shift(x, by):
    count = lax.axis_size("tp")
    return lax.ppermute(x, "tp", [(i, (i + by) % count) for i in range(count)])


def core_swap(x):
    return lax.ppermute(x, "sp", [(i, i ^ 1) for i in range(lax.axis_size("sp"))])


def both(x, pairs):
    sp, tp = lax.axis_size("sp"), lax.axis_size("tp")
    every = []
    for chip in range(sp // 2):
        for (y0, c0), (y1, c1) in pairs:
            every.append(((2 * chip + c0) * tp + y0, (2 * chip + c1) * tp + y1))
    return lax.ppermute(x, ("sp", "tp"), every)


def roles(tp):
    host = [(y, y % 2) for y in range(tp)]
    guest = [(y, 1 - y % 2) for y in range(tp)]
    return host, guest


def weight_routes(tp):
    host, guest = roles(tp)
    over = [(host[y], guest[y]) for y in range(tp)]
    to_left = over + [(guest[y], host[(y - 1) % tp]) for y in range(tp)]
    to_right = over + [(guest[y], host[(y + 1) % tp]) for y in range(tp)]
    return to_left, to_right


def row_routes(tp):
    host, guest = roles(tp)
    first = [(guest[y], host[(y - 1) % tp]) for y in range(tp)]
    first += [(host[y], guest[(y + 2) % tp]) for y in range(tp)]
    second = [(guest[y], host[(y + 1) % tp]) for y in range(tp)]
    second += [(host[y], guest[y]) for y in range(tp)]
    return first, second


def flipped(pairs):
    return [(b, a) for a, b in pairs]


def dot(a, b):
    return jnp.dot(a, b, preferred_element_type=jnp.float32)


def clamped_unit(gate_pre, up_pre):
    gated = jnp.minimum(gate_pre, LIMIT)
    upward = jnp.clip(up_pre, -LIMIT, LIMIT)
    return (upward + 1.0) * gated * jax.nn.sigmoid(ALPHA * gated)


BLOCK = 256
DEPTH = 512
COLUMNS = 512


def blocks(length, size):
    def over(body):
        @pl.loop(0, length // size)
        def _(step):
            body(pl.ds(pl.multiple_of(step * size, size), size))

    return over


def ffn_kernel(rows, gu_low, gu_high, down_low, down_high, out, pre, active):
    count, width = rows.shape
    unit = down_low.shape[0]

    for k, gu in enumerate((gu_low, gu_high)):

        @blocks(count, 64)
        def _(at):
            pre[at, :] = jnp.zeros((at.size, 2 * unit), jnp.float32)

        @blocks(width, DEPTH)
        def _(at):
            pre[...] += dot(rows[:, at], gu[at, :])

        @blocks(count, 32)
        def _(at):
            active[k, at, :] = clamped_unit(pre[at, :unit], pre[at, unit:]).astype(jnp.bfloat16)

    @blocks(width, COLUMNS)
    def _(at):
        total = dot(active[0], down_low[:, at]) + dot(active[1], down_high[:, at])
        out[:, at] = total.astype(out.dtype)


def ffn(rows, low, high):
    number, width = rows.shape
    unit = low[1].shape[0]
    shape = jax.ShapeDtypeStruct((number, width), jnp.bfloat16)
    return pl.pallas_call(
        ffn_kernel,
        out_shape=(shape,),
        in_specs=[pl.BlockSpec(memory_space=pltpu.VMEM)] * 5,
        out_specs=(pl.BlockSpec(memory_space=pltpu.VMEM),),
        scratch_shapes=[
            pltpu.VMEM((number, 2 * unit), jnp.float32),
            pltpu.VMEM((2, number, unit), jnp.bfloat16),
        ],
        compiler_params=pltpu.CompilerParams(vmem_limit_bytes=32 * 2**20),
        cost_estimate=pl.CostEstimate(
            flops=2 * number * width * 6 * unit,
            bytes_accessed=4 * number * width + 12 * unit * width,
            transcendentals=2 * number * unit,
        ),
    )(rows, low[0], high[0], low[1], high[1])


def sum_kernel(a, b, *outs):
    each = outs[0].shape[0]
    for k, out in enumerate(outs):

        @blocks(each, 32)
        def _(at):
            of = pl.ds(k * each + at.start, at.size)
            total = a[of, :].astype(jnp.float32) + b[of, :].astype(jnp.float32)
            out[at, :] = total.astype(out.dtype)


def sum_of(a, b, count=1):
    shape = jax.ShapeDtypeStruct((a.shape[0] // count, a.shape[1]), a.dtype)
    return pl.pallas_call(
        sum_kernel,
        out_shape=(shape,) * count,
        in_specs=[pl.BlockSpec(memory_space=pltpu.VMEM)] * 2,
        out_specs=(pl.BlockSpec(memory_space=pltpu.VMEM),) * count,
        compiler_params=pltpu.CompilerParams(vmem_limit_bytes=8 * 2**20),
        cost_estimate=pl.CostEstimate(
            flops=a.size, bytes_accessed=3 * 2 * a.size, transcendentals=0
        ),
    )(a, b)


def combine_kernel(resid, first, second, places, weight, out, picks):
    shape = picks.shape[1:]
    ids = lax.broadcasted_iota(jnp.int32, shape, 1)
    for at in range(4):
        mine = places[:, at : at + 1] == ids
        picks[at] = jnp.where(mine, 1.0, 0.0).astype(jnp.bfloat16)

    @blocks(resid.shape[1], BLOCK)
    def _(at):
        total = resid[:, at].astype(jnp.float32)
        for k in range(2):
            picked = dot(picks[k], first[:, at]) + dot(picks[2 + k], second[:, at])
            total = total + weight[:, k : k + 1] * picked
        out[:, at] = total.astype(out.dtype)


def combine(resid, first, second, places, weight):
    rows, width = resid.shape
    number = first.shape[0]
    return pl.pallas_call(
        combine_kernel,
        out_shape=jax.ShapeDtypeStruct(resid.shape, resid.dtype),
        in_specs=[pl.BlockSpec(memory_space=pltpu.VMEM)] * 5,
        out_specs=pl.BlockSpec(memory_space=pltpu.VMEM),
        scratch_shapes=[pltpu.VMEM((4, rows, number), jnp.bfloat16)],
        compiler_params=pltpu.CompilerParams(vmem_limit_bytes=16 * 2**20),
        cost_estimate=pl.CostEstimate(
            flops=8 * rows * number * width,
            bytes_accessed=4 * (rows + number) * width,
            transcendentals=0,
        ),
    )(resid, first, second, places, weight)


def fill_kernel(resid, gain, places, *rest):
    *outs, picks = rest
    rows, width = resid.shape
    ids = lax.broadcasted_iota(jnp.int32, picks.shape[1:], 0)
    for c in range(len(outs)):
        mine = (places[2 * c : 2 * c + 1, :] == ids) | (places[2 * c + 1 : 2 * c + 2, :] == ids)
        picks[c] = jnp.where(mine, 1.0, 0.0).astype(jnp.bfloat16)

    def add(step, total):
        at = pl.ds(pl.multiple_of(step * BLOCK, BLOCK), BLOCK)
        part = resid[:, at].astype(jnp.float32)
        return total + jnp.sum(part * part, axis=1, keepdims=True)

    square = lax.fori_loop(0, width // BLOCK, add, jnp.zeros((rows, 1), jnp.float32))
    scale = lax.rsqrt(square / width + EPSILON)

    @blocks(width, BLOCK)
    def _(at):
        normed = resid[:, at].astype(jnp.float32) * scale * gain[:, at]
        normed = normed.astype(jnp.bfloat16)
        for c, out in enumerate(outs):
            out[:, at] = dot(picks[c], normed).astype(out.dtype)


def fill(resid, gain, places, sizes):
    rows, width = resid.shape
    return pl.pallas_call(
        fill_kernel,
        out_shape=tuple(jax.ShapeDtypeStruct((n, width), jnp.bfloat16) for n in sizes),
        in_specs=[pl.BlockSpec(memory_space=pltpu.VMEM)] * 3,
        out_specs=(pl.BlockSpec(memory_space=pltpu.VMEM),) * len(sizes),
        scratch_shapes=[pltpu.VMEM((len(sizes), sizes[0], rows), jnp.bfloat16)],
        compiler_params=pltpu.CompilerParams(vmem_limit_bytes=16 * 2**20),
        cost_estimate=pl.CostEstimate(
            flops=2 * rows * sum(sizes) * width,
            bytes_accessed=2 * (rows + sum(sizes)) * width,
            transcendentals=rows,
        ),
    )(resid, gain, places)


def slots_of(routes, experts):
    rows = routes.shape[0]
    ids = jnp.arange(experts, dtype=jnp.int32)
    first = routes[:, 0:1] == ids
    second = routes[:, 1:2] == ids
    named = (first | second).astype(jnp.bfloat16)
    at = jnp.arange(rows, dtype=jnp.int32)
    earlier = (at[:, None] > at[None, :]).astype(jnp.bfloat16)
    rank = dot(earlier, named)
    ranks = [
        jnp.sum(jnp.where(mine, rank, 0.0), axis=1).astype(jnp.int32) for mine in (first, second)
    ]
    return [routes[:, k] for k in range(2)], ranks


def layer(
    conv_in,
    conv_pre,
    conv_post,
    taps,
    out_proj,
    stream,
    norm_gain,
    routes,
    route_weight,
    gate_w,
    up_w,
    down_w,
):
    sp = lax.axis_size("sp")
    tp = lax.axis_size("tp")
    me = lax.axis_index("tp")
    core = lax.axis_index("sp") % 2
    experts = gate_w.shape[0] * sp
    own_rows, width = stream.shape
    channels = conv_in.shape[1]
    lanes = channels // 2

    mine = lax.dynamic_slice_in_dim(out_proj, core * lanes, lanes, axis=0)
    theirs = lax.dynamic_slice_in_dim(out_proj, (1 - core) * lanes, lanes, axis=0)
    after, before = shift(mine, -1), shift(mine, 1)
    half = lanes // 2
    opposite = jnp.concatenate([shift(after[:half], -1), shift(before[half:], 1)])
    proj = [mine, after, opposite, before]
    unit = gate_w.shape[2] // 2
    halves_of = [
        (jnp.concatenate([gate_w[0, :, cut], up_w[0, :, cut]], axis=1), down_w[0, cut])
        for cut in (slice(0, unit), slice(unit, 2 * unit))
    ]

    edge = jnp.stack([conv_in, conv_pre])
    up = [(i, i + 1) for i in range(sp - 1)]
    prior = lax.ppermute(edge[:, -1:], "sp", up)
    later = lax.ppermute(edge[:, :1], "sp", [(j, i) for i, j in up])
    f32 = jnp.float32
    product = conv_pre.astype(f32) * conv_in.astype(f32)
    padded = jnp.concatenate(
        [
            prior[0].astype(f32) * prior[1].astype(f32),
            product,
            later[0].astype(f32) * later[1].astype(f32),
        ]
    )
    convolved = taps[0] * padded[:-2] + taps[1] * padded[1:-1] + taps[2] * padded[2:]
    mixed = (conv_post.astype(f32) * convolved).astype(jnp.bfloat16)
    low, high = mixed[:, :lanes], mixed[:, lanes:]
    mixed = jnp.concatenate(
        [jnp.where(core == 0, low, high), jnp.where(core == 0, high, low)], axis=1
    )

    def rows_for(d):
        return lax.dynamic_slice_in_dim(mixed, ((me - d) % tp) * own_rows, own_rows, axis=0)

    pieces = [rows_for(0)] + [shift(rows_for(d), -d) for d in range(1, tp)]
    low, high = [
        [both(w, pairs) for w in held] for held, pairs in zip(halves_of, weight_routes(tp))
    ]
    other = {d: core_swap(proj[d]) for d in (1, 3)}
    other[2] = core_swap(opposite)
    other[0] = theirs

    def product_of(d):
        return dot(pieces[d][:, :lanes], proj[d]) + dot(pieces[d][:, lanes:], other[d])

    branch = product_of(0) + product_of(1) + product_of(3)
    branch += product_of(2)

    resid = (stream.astype(f32) + branch).astype(jnp.bfloat16)
    expert_of, rank_of = slots_of(routes, experts)

    firsts = [sum(CHUNKS[:at]) for at in range(len(CHUNKS))]
    places = []
    for first, size in zip(firsts, CHUNKS):
        for e, r in zip(expert_of, rank_of):
            inside = (r >= first) & (r < first + size)
            places.append(jnp.where(inside, e * size + r - first, -1))
    filled = fill(resid, norm_gain[None, :], jnp.stack(places), [experts * size for size in CHUNKS])

    def dispatch(rows, size):
        rows = rows.reshape(experts, size, width)
        arrived = lax.all_to_all(rows, "sp", split_axis=0, concat_axis=0, tiled=True)
        return arrived.reshape(experts * size, width)

    routes_in = row_routes(tp)

    def give_back(arrived, size):
        mine_rows = jnp.concatenate([both(arrived, pairs) for pairs in routes_in])
        their_rows = core_swap(mine_rows)
        (their_out,) = ffn(their_rows, low, high)
        met = core_swap(their_out)
        (my_out,) = ffn(mine_rows, low, high)
        paired = sum_of(my_out, met, 2)
        halves = [both(x, flipped(pairs)) for x, pairs in zip(paired, routes_in)]
        (out,) = sum_of(*halves)
        out = out.reshape(experts, size, width)
        returned = lax.all_to_all(out, "sp", split_axis=0, concat_axis=0, tiled=True)
        return returned.reshape(experts * size, width)

    sent = [dispatch(rows, size) for rows, size in zip(filled, CHUNKS)]
    returned = [give_back(arrived, size) for arrived, size in zip(sent, CHUNKS)]
    return combine(resid, *returned, jnp.stack(places, axis=1), route_weight)


def solution(mesh):
    placed = (
        P("sp", "tp"),
        P("sp", "tp"),
        P("sp", "tp"),
        P(None, "tp"),
        P("tp", None),
        P(("sp", "tp"), None),
        P(),
        P(("sp", "tp"), None),
        P(("sp", "tp"), None),
        P("sp", None, "tp"),
        P("sp", None, "tp"),
        P("sp", "tp", None),
    )
    return jax.shard_map(
        layer, mesh=mesh, in_specs=placed, out_specs=P(("sp", "tp"), None), check_vma=False
    )
```
